32 devices in a mesh: ra: 8 (over z, y), cb: 4 (over x, core).
Axes of the slice: x: 2, y: 2, z: 4, core: 2. Of those that a mesh axis runs over, the one named last changes fastest.
Arguments:
- tokens: bfloat16 [1024, 4096], P(None, 'ra'), may hold values from -40 to 40
- norm_gain: float32 [4096], P('ra'), may hold values from 0.1 to 1.9
- gate_weight: bfloat16 [4096, 11264], P('ra', 'cb'), may hold values from -0.09375 to 0.09375
- up_weight: bfloat16 [4096, 11264], P('ra', 'cb'), may hold values from -0.09375 to 0.09375
- down_weight: bfloat16 [11264, 4096], P('cb', 'ra'), may hold values from -0.0546875 to 0.0546875
- out_gain: float32 [4096], P('ra'), may hold values from 0.1 to 1.9
Outputs:
- normed: bfloat16 [1024, 4096], P(None, 'ra')
The draws below stay inside these ranges and needn't reach their ends.
All inputs are finite; a program needn't handle non-finite values.
Results may differ from the reference program's by a relative error of at most 0.0076.
Values may be sent and summed in bfloat16 or wider, within the bound.
A program may use at most 128 MiB of HBM per device.

```python
import jax
import jax.numpy as jnp
from jax import lax

D = 4096
FF = 11264
TOKENS = 1024


def draw_tokens(key, part):
    keys = jax.random.split(key, 4)
    base = jax.random.normal(keys[0], (TOKENS, D), jnp.float32)
    blocks = jnp.exp(jax.random.uniform(keys[1], (16,), jnp.float32, jnp.log(0.3), jnp.log(3.0)))
    columns = jnp.repeat(blocks, D // 16)[None, :]
    rows = jax.random.uniform(keys[2], (TOKENS, 1), jnp.float32, 0.5, 2.0)
    return jnp.clip(base * columns * rows, -40.0, 40.0).astype(jnp.bfloat16)


def block_scale(key, dims, cuts, smallest, high):
    factor_of = 1.0
    for dim, blocks in cuts:
        heights = jax.random.uniform(jax.random.fold_in(jax.random.fold_in(key, 6), dim), (blocks,), jnp.float32, smallest / len(cuts), high / len(cuts))
        factor_of = factor_of * jnp.repeat(jnp.exp(heights), dims[dim] // blocks).reshape((-1,) + (1,) * (len(dims) - 1 - dim))
    return factor_of


def gaussian(rng, dims, deviation, bound, cuts=(), kind=jnp.bfloat16):
    entries = deviation * jax.random.normal(rng, dims, jnp.float32)
    if cuts:
        entries = entries * block_scale(rng, dims, cuts, -0.22, 0.18)
    return jnp.clip(entries, -bound, bound).astype(kind)


def setup_inputs(seed: int = 0) -> dict:
    key_list = jax.random.split(jax.random.key(seed), 7)
    return {
        "tokens": draw_tokens(jax.random.fold_in(key_list[6], 71), 0),
        "norm_gain": jnp.clip(1.0 + 0.18 * jax.random.normal(key_list[1], (D,), jnp.float32), 0.1, 1.9),
        "gate_weight": gaussian(key_list[2], (D, FF), D ** -0.5, 0.09375, ((0, 8), (1, 4))),
        "up_weight": gaussian(key_list[3], (D, FF), D ** -0.5, 0.09375, ((0, 8), (1, 4))),
        "down_weight": gaussian(key_list[4], (FF, D), FF ** -0.5, 0.0546875, ((0, 4), (1, 8))),
        "out_gain": jnp.clip(1.0 + 0.18 * jax.random.normal(key_list[5], (D,), jnp.float32), 0.1, 1.9),
    }


def reference(tokens, norm_gain, gate_weight, up_weight, down_weight, out_gain):
    stream_in = tokens.astype(jnp.float32)
    inv_rms = jax.lax.rsqrt(lax.optimization_barrier(jnp.sum(stream_in * stream_in, axis=1)) / D + 1e-06)[:, None]
    scaled = (stream_in * norm_gain[None, :]).astype(jnp.bfloat16)
    gate = jnp.dot(scaled, gate_weight, preferred_element_type=jnp.float32) * inv_rms
    up = jnp.dot(scaled, up_weight, preferred_element_type=jnp.float32) * inv_rms
    hidden = (jax.nn.silu(gate) * up).astype(jnp.bfloat16)
    branch = jnp.dot(hidden, down_weight, preferred_element_type=jnp.float32)
    stream = 0.5 * stream_in + branch
    factor = jax.lax.rsqrt(lax.optimization_barrier(jnp.sum(stream * stream, axis=1)) / D + 1e-06)[:, None]
    return (stream * factor * out_gain[None, :]).astype(jnp.bfloat16)
```

```python
import jax
import jax.numpy as jnp
from jax import lax
from jax.sharding import PartitionSpec as P

F32, BF16 = jnp.float32, jnp.bfloat16


def ring_order(mesh):
    n = mesh.shape["ra"]
    column = mesh.devices[:, 0]
    coords = [getattr(d, "coords", None) for d in column]
    if all(c is not None for c in coords):
        ny = len({c[1] for c in coords})
    else:
        ny = 2 if n % 2 == 0 else 1
    nz = n // ny
    if ny == 1 or nz % 2 or nz * ny != n:
        return list(range(n))
    walk = []
    for z in range(nz):
        ys = range(1, ny) if z % 2 == 0 else range(ny - 1, 0, -1)
        walk += [z * ny + y for y in ys]
    return walk + [z * ny for z in reversed(range(nz))]


def butterfly(value, axis, n, narrow=None):
    if n & (n - 1):
        return lax.psum(value, axis)
    step = 1
    while step < n:
        sent = value if narrow is None else value.astype(narrow)
        got = lax.ppermute(sent, axis, [(i, i ^ step) for i in range(n)])
        value = sent.astype(F32) + got.astype(F32)
        step *= 2
    return value


def solution(mesh):
    n_ra, n_cb = mesh.shape["ra"], mesh.shape["cb"]
    order = ring_order(mesh)
    place = [order.index(i) for i in range(n_ra)]
    to_right = [(order[i], order[(i + 1) % n_ra]) for i in range(n_ra)]
    to_left = [(order[i], order[(i - 1) % n_ra]) for i in range(n_ra)]
    far = n_ra // 2

    def body(tokens, norm_gain, gate_weight, up_weight, down_weight, out_gain):
        rows = tokens.shape[0] // n_ra
        width = tokens.shape[1] * n_ra
        hidden_cols = gate_weight.shape[1]
        cut = -(-hidden_cols // 256) * 128
        cols = (slice(0, cut), slice(cut, hidden_cols))
        p = jnp.asarray(place, jnp.int32)[lax.axis_index("ra")]

        def block(array, b):
            start = lax.rem(p + b + n_ra, n_ra) * rows
            return lax.dynamic_slice_in_dim(array, start, rows, 0)

        stream_in = tokens.astype(F32)
        scaled = (stream_in * norm_gain[None, :]).astype(BF16)
        weights = {
            (kind, half): w[:, cols[half]]
            for kind, w in (("g", gate_weight), ("u", up_weight))
            for half in (0, 1)
        }

        def part(key, b):
            return jnp.dot(block(scaled, b), weights[key], preferred_element_type=F32)

        right, left = {}, {}
        for d in range(far, 0, -1):
            for flow, perm, sign, late in ((right, to_right, 1, 1), (left, to_left, -1, 0)):
                for key in weights:
                    if d == far and key[1] == late:
                        continue
                    value = part(key, sign * d)
                    if key in flow:
                        value = value + flow[key].astype(F32)
                    flow[key] = lax.ppermute(value.astype(BF16), "ra", perm)

        sq = butterfly(jnp.sum(stream_in * stream_in, axis=1), "ra", n_ra)
        inv_rms = lax.rsqrt(block(sq, 0) / width + 1e-06)[:, None]

        own = []
        for half in (0, 1):
            total = {}
            for kind in ("g", "u"):
                key = (kind, half)
                value = part(key, 0)
                for flow in (right, left):
                    if key in flow:
                        value = value + flow[key].astype(F32)
                total[kind] = value * inv_rms
            own.append((jax.nn.silu(total["g"]) * total["u"]).astype(BF16))

        stream = jnp.zeros(tokens.shape, F32)
        sums = jnp.zeros(tokens.shape[:1], F32)

        def finish(stream, sums, held):
            halves = [jnp.concatenate([h[i] for _, h in held], axis=0) for i in (0, 1)]
            down = sum(
                jnp.dot(halves[i], down_weight[cols[i]], preferred_element_type=F32) for i in (0, 1)
            )
            branch = butterfly(down, "cb", n_cb, BF16)
            for i, (b, _) in enumerate(held):
                new = 0.5 * block(stream_in, b) + branch[i * rows : (i + 1) * rows]
                start = lax.rem(p + b + n_ra, n_ra) * rows
                stream = lax.dynamic_update_slice_in_dim(stream, new, start, 0)
                sums = lax.dynamic_update_slice_in_dim(sums, jnp.sum(new * new, axis=1), start, 0)
            return stream, sums

        from_left, from_right = list(own), list(own)
        pending = [(0, own)]
        for s in range(1, far + 1):
            last = s == far
            new_left = [
                None if last and h else lax.ppermute(from_left[h], "ra", to_right) for h in (0, 1)
            ]
            new_right = [
                None if last and not h else lax.ppermute(from_right[h], "ra", to_left) for h in (0, 1)
            ]
            stream, sums = finish(stream, sums, pending)
            if last:
                pending = [(far, [new_left[0], new_right[1]])]
            else:
                pending = [(-s, new_left), (s, new_right)]
            from_left, from_right = new_left, new_right
        stream, sums = finish(stream, sums, pending)

        total_sq = butterfly(sums, "ra", n_ra)
        factor = lax.rsqrt(total_sq / width + 1e-06)[:, None]
        return (stream * factor * out_gain[None, :]).astype(BF16)

    placed = (P(None, "ra"), P("ra"), P("ra", "cb"), P("ra", "cb"), P("cb", "ra"), P("ra"))
    return jax.shard_map(body, mesh=mesh, in_specs=placed, out_specs=P(None, "ra"), check_vma=False)
```

```python
import jax
import jax.numpy as jnp
from jax import lax
from jax.sharding import PartitionSpec as P

F32, BF16 = jnp.float32, jnp.bfloat16


def ring_order(mesh):
    n = mesh.shape["ra"]
    column = mesh.devices[:, 0]
    coords = [getattr(d, "coords", None) for d in column]
    if all(c is not None for c in coords):
        ny = len({c[1] for c in coords})
    else:
        ny = 2 if n % 2 == 0 else 1
    nz = n // ny
    if ny == 1 or nz % 2 or nz * ny != n:
        return list(range(n))
    walk = []
    for z in range(nz):
        ys = range(1, ny) if z % 2 == 0 else range(ny - 1, 0, -1)
        walk += [z * ny + y for y in ys]
    return walk + [z * ny for z in reversed(range(nz))]


def butterfly(value, axis, n, narrow=None):
    if n & (n - 1):
        return lax.psum(value, axis)
    step = 1
    while step < n:
        sent = value if narrow is None else value.astype(narrow)
        got = lax.ppermute(sent, axis, [(i, i ^ step) for i in range(n)])
        value = sent.astype(F32) + got.astype(F32)
        step *= 2
    return value


def solution(mesh):
    n_ra, n_cb = mesh.shape["ra"], mesh.shape["cb"]
    order = ring_order(mesh)
    place = [order.index(i) for i in range(n_ra)]
    to_right = [(order[i], order[(i + 1) % n_ra]) for i in range(n_ra)]
    to_left = [(order[i], order[(i - 1) % n_ra]) for i in range(n_ra)]
    far = n_ra // 2

    def body(tokens, norm_gain, gate_weight, up_weight, down_weight, out_gain):
        rows = tokens.shape[0] // n_ra
        width = tokens.shape[1] * n_ra
        hidden_cols = gate_weight.shape[1]
        cut = -(-hidden_cols // 256) * 128
        cols = (slice(0, cut), slice(cut, hidden_cols))
        p = jnp.asarray(place, jnp.int32)[lax.axis_index("ra")]

        def block(array, b):
            start = lax.rem(p + b + n_ra, n_ra) * rows
            return lax.dynamic_slice_in_dim(array, start, rows, 0)

        stream_in = tokens.astype(F32)
        scaled = (stream_in * norm_gain[None, :]).astype(BF16)
        weights = {"g": gate_weight, "u": up_weight}

        def parts(source, offsets):
            x = jnp.concatenate([block(source, b) for b in offsets], axis=0)
            return {k: jnp.dot(x, w, preferred_element_type=F32) for k, w in weights.items()}

        right, left = {}, {}
        source = scaled
        for d in range(far, 0, -1):
            mine = parts(source, (d,) if d == far else (d, -d))
            if d < far:
                source, right["g"] = lax.optimization_barrier((source, right["g"]))
            for key in ("g", "u"):
                for flow, perm, skip, at in ((right, to_right, "u", 0), (left, to_left, "g", rows)):
                    if d == far and key == skip:
                        continue
                    value = mine[key] if d == far else mine[key][at : at + rows]
                    if key in flow:
                        value = value + flow[key].astype(F32)
                    flow[key] = lax.ppermute(value.astype(BF16), "ra", perm)
        mine = parts(source, (0,))

        sq = butterfly(jnp.sum(stream_in * stream_in, axis=1), "ra", n_ra)
        inv_rms = lax.rsqrt(block(sq, 0) / width + 1e-06)[:, None]

        total = {}
        for key in ("g", "u"):
            value = mine[key]
            for flow in (right, left):
                if key in flow:
                    value = value + flow[key].astype(F32)
            total[key] = value * inv_rms
        own = (jax.nn.silu(total["g"]) * total["u"]).astype(BF16)

        stream = jnp.zeros(tokens.shape, F32)
        sums = jnp.zeros(tokens.shape[:1], F32)

        def finish(stream, sums, held):
            units = jnp.concatenate([h for _, h in held], axis=0)
            down = jnp.dot(units, down_weight, preferred_element_type=F32)
            branch = butterfly(down, "cb", n_cb, BF16)
            for i, (b, _) in enumerate(held):
                new = 0.5 * block(stream_in, b) + branch[i * rows : (i + 1) * rows]
                start = lax.rem(p + b + n_ra, n_ra) * rows
                stream = lax.dynamic_update_slice_in_dim(stream, new, start, 0)
                sums = lax.dynamic_update_slice_in_dim(sums, jnp.sum(new * new, axis=1), start, 0)
            return stream, sums

        from_left = from_right = own
        pending = [(0, own)]
        for s in range(1, far + 1):
            last = s == far
            if last:
                from_left, from_right = from_left[:, cols[0]], from_right[:, cols[1]]
            from_left = lax.ppermute(from_left, "ra", to_right)
            from_right = lax.ppermute(from_right, "ra", to_left)
            stream, sums = finish(stream, sums, pending)
            if last:
                pending = [(far, jnp.concatenate([from_left, from_right], axis=1))]
            else:
                pending = [(-s, from_left), (s, from_right)]
        stream, sums = finish(stream, sums, pending)

        total_sq = butterfly(sums, "ra", n_ra)
        factor = lax.rsqrt(total_sq / width + 1e-06)[:, None]
        return (stream * factor * out_gain[None, :]).astype(BF16)

    placed = (P(None, "ra"), P("ra"), P("ra", "cb"), P("ra", "cb"), P("cb", "ra"), P("ra"))
    return jax.shard_map(body, mesh=mesh, in_specs=placed, out_specs=P(None, "ra"), check_vma=False)
```

```python
import jax
import jax.numpy as jnp
from jax import lax
from jax.sharding import PartitionSpec as P

F32, BF16 = jnp.float32, jnp.bfloat16


def ring_order(mesh):
    n = mesh.shape["ra"]
    column = mesh.devices[:, 0]
    coords = [getattr(d, "coords", None) for d in column]
    if all(c is not None for c in coords):
        ny = len({c[1] for c in coords})
    else:
        ny = 2 if n % 2 == 0 else 1
    nz = n // ny
    if ny == 1 or nz % 2 or nz * ny != n:
        return list(range(n))
    walk = []
    for z in range(nz):
        ys = range(1, ny) if z % 2 == 0 else range(ny - 1, 0, -1)
        walk += [z * ny + y for y in ys]
    return walk + [z * ny for z in reversed(range(nz))]


def butterfly(value, axis, n, narrow=None):
    if n & (n - 1):
        return lax.psum(value, axis)
    step = 1
    while step < n:
        sent = value if narrow is None else value.astype(narrow)
        got = lax.ppermute(sent, axis, [(i, i ^ step) for i in range(n)])
        value = sent.astype(F32) + got.astype(F32)
        step *= 2
    return value


def solution(mesh):
    n_ra, n_cb = mesh.shape["ra"], mesh.shape["cb"]
    order = ring_order(mesh)
    place = [order.index(i) for i in range(n_ra)]
    to_right = [(order[i], order[(i + 1) % n_ra]) for i in range(n_ra)]
    to_left = [(order[i], order[(i - 1) % n_ra]) for i in range(n_ra)]
    far = n_ra // 2

    def body(tokens, norm_gain, gate_weight, up_weight, down_weight, out_gain):
        rows = tokens.shape[0] // n_ra
        width = tokens.shape[1] * n_ra
        hidden_cols = gate_weight.shape[1]
        cut = -(-hidden_cols // 256) * 128
        cols = (slice(0, cut), slice(cut, hidden_cols))
        p = jnp.asarray(place, jnp.int32)[lax.axis_index("ra")]

        def block(array, b):
            start = lax.rem(p + b + n_ra, n_ra) * rows
            return lax.dynamic_slice_in_dim(array, start, rows, 0)

        stream_in = tokens.astype(F32)
        scaled = (stream_in * norm_gain[None, :]).astype(BF16)
        weights = {"g": gate_weight, "u": up_weight}

        def parts(source, offsets):
            x = jnp.concatenate([block(source, b) for b in offsets], axis=0)
            return {k: jnp.dot(x, w, preferred_element_type=F32) for k, w in weights.items()}

        right, left = {}, {}
        source = scaled
        for d in range(far, 0, -1):
            mine = parts(source, (d,) if d == far else (d, -d))
            if d < far:
                source, right["g"] = lax.optimization_barrier((source, right["g"]))
            for key in ("g", "u"):
                for flow, perm, skip, at in ((right, to_right, "u", 0), (left, to_left, "g", rows)):
                    if d == far and key == skip:
                        continue
                    value = mine[key] if d == far else mine[key][at : at + rows]
                    if key in flow:
                        value = value + flow[key].astype(F32)
                    flow[key] = lax.ppermute(value.astype(BF16), "ra", perm)
        mine = parts(source, (0,))

        squares = jnp.sum(stream_in * stream_in, axis=1)
        sq = block(squares, 0)
        for k in range(1, n_ra):
            perm = [(order[i], order[(i + k) % n_ra]) for i in range(n_ra)]
            sq = sq + lax.ppermute(block(squares, k), "ra", perm)
        inv_rms = lax.rsqrt(sq / width + 1e-06)[:, None]

        total = {}
        for key in ("g", "u"):
            value = mine[key]
            for flow in (right, left):
                if key in flow:
                    value = value + flow[key].astype(F32)
            total[key] = value * inv_rms
        own = (jax.nn.silu(total["g"]) * total["u"]).astype(BF16)

        stream = jnp.zeros(tokens.shape, F32)
        sums = jnp.zeros(tokens.shape[:1], F32)

        def finish(stream, sums, held):
            units = jnp.concatenate([h for _, h in held], axis=0)
            down = jnp.dot(units, down_weight, preferred_element_type=F32)
            branch = butterfly(down, "cb", n_cb, BF16)
            for i, (b, _) in enumerate(held):
                new = 0.5 * block(stream_in, b) + branch[i * rows : (i + 1) * rows]
                start = lax.rem(p + b + n_ra, n_ra) * rows
                stream = lax.dynamic_update_slice_in_dim(stream, new, start, 0)
                sums = lax.dynamic_update_slice_in_dim(sums, jnp.sum(new * new, axis=1), start, 0)
            return stream, sums

        from_left = from_right = own
        pending = [(0, own)]
        for s in range(1, far + 1):
            last = s == far
            if last:
                from_left, from_right = from_left[:, cols[0]], from_right[:, cols[1]]
            from_left = lax.ppermute(from_left, "ra", to_right)
            from_right = lax.ppermute(from_right, "ra", to_left)
            stream, sums = finish(stream, sums, pending)
            if last:
                pending = [(far, jnp.concatenate([from_left, from_right], axis=1))]
            else:
                pending = [(-s, from_left), (s, from_right)]
        stream, sums = finish(stream, sums, pending)

        total_sq = butterfly(sums, "ra", n_ra)
        factor = lax.rsqrt(total_sq / width + 1e-06)[:, None]
        return (stream * factor * out_gain[None, :]).astype(BF16)

    placed = (P(None, "ra"), P("ra"), P("ra", "cb"), P("ra", "cb"), P("cb", "ra"), P("ra"))
    return jax.shard_map(body, mesh=mesh, in_specs=placed, out_specs=P(None, "ra"), check_vma=False)
```
